256 devices in a mesh: grp: 4 (over y, x), ep: 64 (over z, core).
Axes of the slice: x: 2, y: 2, z: 32, core: 2. Of those that a mesh axis runs over, the one named last changes fastest.
The devices are a block of a 4x8x32 slice.
Arguments:
- tokens: bfloat16 [65536, 2048], P(('grp', 'ep')), parts along dimension 0, may hold values from -6 to 6
- norm_gain: float32 [2048], replicated, may hold values from 0.1 to 1.9
- routes: int32 [65536, 2], P(('grp', 'ep')), parts along dimension 0, may hold values from 0 to 63, all different within a row; in each aligned block of 256 rows (0 to 255, 256 to 511, ...) at most 10 rows name the same one
- route_weights: float32 [65536, 2], P(('grp', 'ep')), parts along dimension 0, may hold values from 0.2 to 1.5
- expert_gate: bfloat16 [64, 2048, 256], P('ep'), may hold values from -0.125 to 0.125
- expert_up: bfloat16 [64, 2048, 256], P('ep'), may hold values from -0.125 to 0.125
- expert_down: bfloat16 [64, 256, 2048], P('ep'), may hold values from -0.375 to 0.375
- shared_gate: bfloat16 [2048, 256], replicated, may hold values from -0.125 to 0.125
- shared_up: bfloat16 [2048, 256], replicated, may hold values from -0.125 to 0.125
- shared_down: bfloat16 [256, 2048], replicated, may hold values from -0.375 to 0.375
Outputs:
- mixed: bfloat16 [65536, 2048], P(('grp', 'ep')), parts along dimension 0
The draws below stay inside these ranges and needn't reach their ends.
There are 4 independent parts, one for each index of `grp`. The reference program is written for one: setup_inputs(seed, part) draws one part's arguments, and reference() takes and returns one part's arrays. A program takes and returns all parts, laid end to end along the dimension named above; an argument that names none is the same for every part. Nothing has to cross between parts.
Inputs may be any that keep to these rules, and one draw needn't show every extreme that they name: `routes`: the 2 experts of a token are distinct. Among the tokens of one device, at most 10 choose any one expert; in every draw some expert is chosen by exactly 10 tokens of some device.
All inputs are finite; a program needn't handle non-finite values.
Results may differ from the reference program's by a relative error of at most 0.0075.
Values may be sent and summed in bfloat16 or wider, within the bound.
No kernel may reach another device: no remote copies, remote signals or barrier semaphores. Data moves between devices by JAX's collectives and lax.ppermute only.
A program may use at most 64 MiB of HBM per device.

```python
import math
import jax
import jax.numpy as jnp
import numpy as np
from jax import lax

D = 2048
DE = 256
DS = 256
TOP_K = 2
TOK_DEV = 256
EXPERTS = 64
TOKENS = 16384
CAPACITY = 10
N_EP = 64


def block_levels(key, dims, cuts, least, largest):
    loudness, own = 1.0, jax.random.fold_in(key, 6)
    for dim, parts in cuts:
        draws = jnp.exp(jax.random.uniform(jax.random.fold_in(own, dim), (parts,), jnp.float32, least / len(cuts), largest / len(cuts)))
        loudness = loudness * jnp.repeat(draws, dims[dim] // parts).reshape([-1 if axis == dim else 1 for axis in range(len(dims))])
    return loudness


def routed_block(key, own, number, rows, amount, top, most, skew):
    sequence = jax.random.permutation(key, amount)
    heavy_load, common = load_shares(amount, rows * top, most, skew, True), load_shares(amount, rows * top, most, skew, False)
    places = jnp.arange(amount)

    def named(tallies, rotation):
        used = int((tallies > 0).sum())
        fixed = max(1, used // 4)
        passed = fixed + (places - fixed + rotation * (used - fixed)) % max(1, amount - fixed)
        return jnp.zeros((amount,), jnp.int32).at[sequence[jnp.where(places < fixed, places, passed)]].set(jnp.asarray(tallies, jnp.int32))

    tallies = jnp.where(number % 4 == 0, named(heavy_load, number // 4), named(common, number - number // 4 - 1))
    mixed = jax.random.permutation(jax.random.fold_in(own, 3), amount)
    source_of, taker = mixed[0:amount // 2 * 2:2], mixed[1:amount // 2 * 2:2]
    room = jnp.minimum(tallies[source_of] - 1, most - tallies[taker]) // 2
    room = jnp.where((source_of == sequence[0]) | (taker == sequence[0]) | (tallies[taker] == 0), 0, jnp.maximum(room, 0))
    passed = jax.random.randint(jax.random.fold_in(own, 4), (amount // 2,), 0, 1 << 20) % (room + 1)
    tallies = tallies.at[source_of].add(-passed).at[taker].add(passed)
    labels = jnp.searchsorted(jnp.cumsum(tallies), jnp.arange(rows * top), side="right").astype(jnp.int32)
    table = labels.reshape(top, rows).T
    table = table[jax.random.permutation(jax.random.fold_in(own, 1), rows)]
    rotation = jax.random.randint(jax.random.fold_in(own, 2), (rows, 1), 0, top)
    return jnp.take_along_axis(table, (jnp.arange(top)[None, :] + rotation) % top, axis=1)


def load_shares(number_of, total, reach, skew, full):
    weights = [(1 << 20) // math.isqrt(grade ** skew) + 1 for grade in range(1, number_of + 1)]
    largest = reach if full else min(reach, max(-(-total // number_of), total * weights[0] // sum(weights)))
    least = 1 if total - largest >= number_of - 1 else 0
    holding, rest = [largest] + [least] * (number_of - 1), total - largest - least * (number_of - 1)
    while rest > 0:
        movable = [i for i in range(1, number_of) if holding[i] < largest] or [i for i in range(1, number_of) if holding[i] < reach]
        whole, left = sum([weights[i] for i in movable]), rest
        for i in movable:
            addition = min(reach - holding[i], max(1, left * weights[i] // whole), rest)
            holding[i] = holding[i] + addition
            rest = rest - addition
    return np.array(holding)


def centred(own_key, dims, spread, limit, shards=(), kind=jnp.bfloat16):
    values = spread * jax.random.normal(own_key, dims, jnp.float32)
    if shards:
        values = values * block_levels(own_key, dims, shards, -0.22, 0.18)
    return jnp.clip(values, -limit, limit).astype(kind)


def setup_inputs(seed: int = 0, part: int = 0) -> dict:
    key_of = jax.random.split(jax.random.key(seed), 11)
    own_keys = jax.random.split(jax.random.fold_in(key_of[10], part), 11)
    tokens = centred(own_keys[0], (TOKENS, D), 1.0, 6.0, ((0, 64),))
    norm_gain = jnp.clip(1.0 + 0.18 * jax.random.normal(key_of[1], (D,), jnp.float32), 0.1, 1.9)
    routes_keys = jax.random.split(jax.random.fold_in(own_keys[2], 1), TOKENS // TOK_DEV)
    routes_turns = jax.random.permutation(jax.random.fold_in(own_keys[2], 3), TOKENS // TOK_DEV)
    routes = jax.vmap(lambda own, number: routed_block(jax.random.fold_in(own_keys[2], 2), own, number, TOK_DEV, EXPERTS, TOP_K, CAPACITY, 2))(routes_keys, routes_turns).reshape((TOKENS, TOP_K))
    route_weights = jnp.clip(0.2 + 1.3 * jax.random.uniform(own_keys[3], (TOKENS, TOP_K), jnp.float32) ** block_levels(own_keys[3], (TOKENS, TOP_K), ((0, 64),), -0.2, 0.2), 0.2, 1.5)
    expert_gate = centred(key_of[4], (EXPERTS, D, DE), D ** -0.5, 0.125, ((0, 64),))
    expert_up = centred(key_of[5], (EXPERTS, D, DE), D ** -0.5, 0.125, ((0, 64),))
    expert_down = centred(key_of[6], (EXPERTS, DE, D), DE ** -0.5, 0.375, ((0, 64),))
    shared_gate = centred(key_of[7], (D, DS), D ** -0.5, 0.125)
    shared_up = centred(key_of[8], (D, DS), D ** -0.5, 0.125)
    shared_down = centred(key_of[9], (DS, D), DS ** -0.5, 0.375)
    return dict(tokens=tokens, norm_gain=norm_gain, routes=routes, route_weights=route_weights, expert_gate=expert_gate, expert_up=expert_up, expert_down=expert_down, shared_gate=shared_gate, shared_up=shared_up, shared_down=shared_down)


def swiglu_rows(row_block, w_gate, w_up, w_down):
    gate_part = jnp.dot(row_block, w_gate, preferred_element_type=jnp.float32)
    up_part = jnp.dot(row_block, w_up, preferred_element_type=jnp.float32)
    hidden = (jax.nn.silu(gate_part) * up_part).astype(jnp.bfloat16)
    return jnp.dot(hidden, w_down, preferred_element_type=jnp.float32)

def reference(tokens, norm_gain, routes, route_weights, expert_gate, expert_up, expert_down, shared_gate, shared_up, shared_down):
    upcast = tokens.astype(jnp.float32)
    factor = lax.rsqrt(lax.optimization_barrier(jnp.mean(upcast * upcast, axis=-1, keepdims=True)) + 1e-06)
    normed = (upcast * factor * norm_gain.astype(jnp.float32)).astype(jnp.bfloat16)
    pair_count = TOKENS * TOP_K
    flat_expert = routes.reshape(-1).astype(jnp.int32)
    onehot = (flat_expert[:, None] == jnp.arange(EXPERTS, dtype=jnp.int32)[None, :]).astype(jnp.int32)
    position = (lax.optimization_barrier(jnp.sum(jnp.cumsum(onehot, axis=0) * onehot, axis=1)) - 1).astype(jnp.int32)
    per_expert = N_EP * CAPACITY
    slot_index = (flat_expert * per_expert + position).astype(jnp.int32)
    pair_token = (jnp.arange(pair_count, dtype=jnp.int32) // TOP_K).astype(jnp.int32)
    slot_token = jnp.full((EXPERTS * per_expert,), TOKENS, jnp.int32).at[slot_index].set(pair_token)
    padded = jnp.concatenate([normed, jnp.zeros((1, D), jnp.bfloat16)], axis=0)

    def one_expert(args):
        table, w_gate, w_up, w_down = args
        return swiglu_rows(padded[table], w_gate, w_up, w_down).astype(jnp.bfloat16)
    outputs = lax.map(one_expert, (slot_token.reshape(EXPERTS, per_expert), expert_gate, expert_up, expert_down))
    pair_out = outputs.reshape(EXPERTS * per_expert, D)[slot_index].astype(jnp.float32).reshape(TOKENS, TOP_K, D)
    routed = lax.optimization_barrier(jnp.sum(pair_out * route_weights[:, :, None], axis=1))
    shared = swiglu_rows(normed, shared_gate, shared_up, shared_down)
    return (routed + shared).astype(jnp.bfloat16)
```

```python
import jax
import jax.numpy as jnp
from jax import lax
from jax.sharding import PartitionSpec as P


def swiglu_rows(row_block, w_gate, w_up, w_down):
    gate_part = jnp.dot(row_block, w_gate, preferred_element_type=jnp.float32)
    up_part = jnp.dot(row_block, w_up, preferred_element_type=jnp.float32)
    hidden = (jax.nn.silu(gate_part) * up_part).astype(jnp.bfloat16)
    return jnp.dot(hidden, w_down, preferred_element_type=jnp.float32)


def on_device(
    tokens,
    norm_gain,
    routes,
    route_weights,
    expert_gate,
    expert_up,
    expert_down,
    shared_gate,
    shared_up,
    shared_down,
):
    tok_rows, model_width = tokens.shape
    top_count = routes.shape[1]
    devices_ep = lax.axis_size("ep")
    capacity = 5 * tok_rows * top_count // (4 * devices_ep)
    upcast = tokens.astype(jnp.float32)
    factor = lax.rsqrt(jnp.mean(upcast * upcast, axis=-1, keepdims=True) + 1e-06)
    normed = (upcast * factor * norm_gain).astype(jnp.bfloat16)
    flat_expert = routes.reshape(-1)
    onehot = (flat_expert[:, None] == jnp.arange(devices_ep, dtype=jnp.int32)[None, :]).astype(
        jnp.int32
    )
    position = jnp.sum(jnp.cumsum(onehot, axis=0) * onehot, axis=1) - 1
    slot_index = flat_expert * capacity + position
    pair_token = jnp.arange(tok_rows * top_count, dtype=jnp.int32) // top_count
    slot_token = (
        jnp.full((devices_ep * capacity,), tok_rows, jnp.int32).at[slot_index].set(pair_token)
    )
    padded = jnp.concatenate([normed, jnp.zeros((1, model_width), jnp.bfloat16)], axis=0)
    outgoing = padded[slot_token].reshape(devices_ep, 160, 128)
    arrived = lax.all_to_all(outgoing, "ep", split_axis=0, concat_axis=0, tiled=True)
    flat_rows = arrived.reshape(devices_ep * capacity, model_width)
    expert_rows = swiglu_rows(flat_rows, expert_gate[0], expert_up[0], expert_down[0]).astype(
        jnp.bfloat16
    )
    returned = lax.all_to_all(
        expert_rows.reshape(devices_ep, 160, 128),
        "ep",
        split_axis=0,
        concat_axis=0,
        tiled=True,
    )
    pair_out = returned.reshape(devices_ep * capacity, model_width)[slot_index]
    pair_out = pair_out.reshape(tok_rows, top_count, model_width)
    routed = jnp.einsum("tk,tkd->td", route_weights, pair_out.astype(jnp.float32))
    shared_result = swiglu_rows(normed, shared_gate, shared_up, shared_down)
    return (routed + shared_result).astype(jnp.bfloat16)


def solution(mesh):
    return jax.shard_map(
        on_device,
        mesh=mesh,
        in_specs=(
            P(("grp", "ep"), None),
            P(),
            P(("grp", "ep"), None),
            P(("grp", "ep"), None),
            P("ep", None, None),
            P("ep", None, None),
            P("ep", None, None),
            P(),
            P(),
            P(),
        ),
        out_specs=P(("grp", "ep"), None),
        check_vma=False,
    )
```

```python
import jax
import jax.numpy as jnp
from jax import lax
from jax.experimental import pallas as pl
from jax.experimental.pallas import tpu as pltpu
from jax.sharding import PartitionSpec as P


BLOCK = 4
CORES = 2
LIMIT = 48 * 1024 * 1024


def swiglu_rows(row_block, w_gate, w_up, w_down):
    gate_part = jnp.dot(row_block, w_gate, preferred_element_type=jnp.float32)
    up_part = jnp.dot(row_block, w_up, preferred_element_type=jnp.float32)
    hidden = (jax.nn.silu(gate_part) * up_part).astype(jnp.bfloat16)
    return jnp.dot(hidden, w_down, preferred_element_type=jnp.float32)


def call(body, out_shape, name, flops):
    return pl.pallas_call(
        body,
        out_shape=out_shape,
        name=name,
        compiler_params=pltpu.CompilerParams(vmem_limit_bytes=LIMIT),
        cost_estimate=pl.CostEstimate(flops=flops, bytes_accessed=8 << 20, transcendentals=0),
    )


def select_rows(normed, slots, count, rows):
    width = normed.shape[1]

    def body(slots_ref, normed_ref, *outs):
        slot_a, slot_b = slots_ref[0:1, :], slots_ref[1:2, :]
        for s in range(count):
            row = lax.broadcasted_iota(jnp.int32, (rows, normed.shape[0]), 0) + s * rows
            pick = jnp.where((row == slot_a) | (row == slot_b), 1.0, 0.0).astype(jnp.bfloat16)
            outs[s][...] = jnp.dot(pick, normed_ref[...], preferred_element_type=jnp.float32).astype(jnp.bfloat16)

    out = [jax.ShapeDtypeStruct((rows, width), jnp.bfloat16)] * count
    return call(body, out, "select_rows", 2 * count * rows * normed.shape[0] * width)(slots, normed)


def expert_rows(arrived, source, weights, hidden_width):
    width = arrived[0].shape[1]
    total = len(arrived) * arrived[0].shape[0]
    rows = source.shape[0]

    def body(source_ref, weights_ref, *refs):
        out = refs[-1]
        everything = jnp.concatenate([ref[...] for ref in refs[:-1]], axis=0)
        column = lax.broadcasted_iota(jnp.int32, (rows, total), 1)
        pick = jnp.where(column == source_ref[...], 1.0, 0.0).astype(jnp.bfloat16)
        mine = jnp.dot(pick, everything, preferred_element_type=jnp.float32).astype(jnp.bfloat16)
        gate = jnp.dot(mine, weights_ref[0:width, :], preferred_element_type=jnp.float32)
        up = jnp.dot(mine, weights_ref[width : 2 * width, :], preferred_element_type=jnp.float32)
        hidden = (gate / (1.0 + jnp.exp(-gate)) * up).astype(jnp.bfloat16)
        for b in range(width // hidden_width):
            start = 2 * width + b * hidden_width
            down = weights_ref[start : start + hidden_width, :]
            part = jnp.dot(hidden, down, preferred_element_type=jnp.float32)
            out[:, b * hidden_width : (b + 1) * hidden_width] = part.astype(jnp.bfloat16)

    out = jax.ShapeDtypeStruct((rows, width), jnp.bfloat16)
    flops = 2 * rows * width * (total + 3 * hidden_width)
    return call(body, out, "expert_rows", flops)(source, weights, *arrived)


def reorder_rows(results, source, count, rows):
    width = results[0].shape[1]
    total = len(results) * results[0].shape[0]

    def body(source_ref, *refs):
        everything = jnp.concatenate([ref[...] for ref in refs[: len(results)]], axis=0)
        for s in range(count):
            column = lax.broadcasted_iota(jnp.int32, (rows, total), 1)
            pick = jnp.where(column == source_ref[s * rows : (s + 1) * rows, :], 1.0, 0.0).astype(jnp.bfloat16)
            picked = jnp.dot(pick, everything, preferred_element_type=jnp.float32)
            refs[len(results) + s][...] = picked.astype(jnp.bfloat16)

    out = [jax.ShapeDtypeStruct((rows, width), jnp.bfloat16)] * count
    return call(body, out, "reorder_rows", 2 * count * rows * total * width)(source, *results)


def mix_rows(returned, slots, factors, shared_result):
    width = returned[0].shape[1]
    total = len(returned) * returned[0].shape[0]
    tok_rows, top_count = slots.shape

    def body(slots_ref, factors_ref, shared_ref, *refs):
        everything = jnp.concatenate([ref[...] for ref in refs[:-1]], axis=0)
        column = lax.broadcasted_iota(jnp.int32, (tok_rows, total), 1)
        spread = jnp.zeros((tok_rows, total), jnp.float32)
        for k in range(top_count):
            spread = spread + jnp.where(column == slots_ref[:, k : k + 1], factors_ref[:, k : k + 1], 0.0)
        high = spread.astype(jnp.bfloat16)
        low = (spread - high.astype(jnp.float32)).astype(jnp.bfloat16)
        routed = jnp.dot(high, everything, preferred_element_type=jnp.float32)
        routed = routed + jnp.dot(low, everything, preferred_element_type=jnp.float32)
        refs[-1][...] = (routed + shared_ref[...]).astype(jnp.bfloat16)

    out = jax.ShapeDtypeStruct((tok_rows, width), jnp.bfloat16)
    return call(body, out, "mix_rows", 4 * tok_rows * total * width)(slots, factors, shared_result, *returned)


def on_device(
    tokens,
    norm_gain,
    routes,
    route_weights,
    expert_gate,
    expert_up,
    expert_down,
    shared_gate,
    shared_up,
    shared_down,
):
    tok_rows, model_width = tokens.shape
    top_count = routes.shape[1]
    hidden_width = expert_gate.shape[2]
    devices_ep = lax.axis_size("ep")
    groups = lax.axis_size("grp")
    capacity = 5 * tok_rows * top_count // (4 * devices_ep)
    chips = devices_ep // CORES
    copies = chips // BLOCK
    hosts = BLOCK * CORES
    slots_host = copies * capacity
    me = lax.axis_index("ep")
    chip, core = me // CORES, me % CORES
    member = chip // BLOCK

    down_blocks = [expert_down[0, :, b * hidden_width : (b + 1) * hidden_width] for b in range(model_width // hidden_width)]
    stacked = jnp.concatenate([expert_gate[0], expert_up[0], *down_blocks], axis=0)
    share_rows = stacked.shape[0] // groups
    share = lax.dynamic_slice_in_dim(stacked, lax.axis_index("grp") * share_rows, share_rows, 0)

    onward = [(d, (d + (hosts if d % CORES == 0 else -hosts)) % devices_ep) for d in range(devices_ep)]
    pieces = [share]
    for _ in range(copies - 1):
        pieces.append(lax.ppermute(pieces[-1], "ep", onward))
    whole = [lax.all_gather(piece, "grp", axis=0, tiled=True) for piece in pieces]

    upcast = tokens.astype(jnp.float32)
    factor = lax.rsqrt(jnp.mean(upcast * upcast, axis=-1, keepdims=True) + 1e-06)
    normed = (upcast * factor * norm_gain).astype(jnp.bfloat16)

    flat_expert = routes.reshape(-1)
    onehot = (flat_expert[:, None] == jnp.arange(devices_ep, dtype=jnp.int32)[None, :]).astype(jnp.int32)
    position = jnp.sum(jnp.cumsum(onehot, axis=0) * onehot, axis=1) - 1
    expert_chip = flat_expert // CORES
    turn = (expert_chip - chip) % BLOCK
    host = turn * CORES + (flat_expert + core) % CORES
    slot = host * slots_host + (expert_chip // BLOCK) * capacity + position
    slots = slot.reshape(tok_rows, top_count)

    def host_of(d, h):
        z, c = d // CORES, d % CORES
        turn, swap = h // CORES, h % CORES
        half = BLOCK // 2
        move = turn - BLOCK if turn > half or (turn == half and c == 1) else turn
        return (z + move) % chips * CORES + (c + swap) % CORES

    outgoing = select_rows(normed, slots.T, hosts, slots_host)
    arrived, back = [], []
    for h in range(hosts):
        there = [(d, host_of(d, h)) for d in range(devices_ep)]
        back.append([(b, a) for a, b in there])
        arrived.append(outgoing[h] if h == 0 else lax.ppermute(outgoing[h], "ep", there))

    shared_result = swiglu_rows(normed, shared_gate, shared_up, shared_down)

    taken = hosts * capacity
    line = jnp.arange(taken, dtype=jnp.int32)[:, None]
    results = []
    towards = 1 - 2 * core
    for away, weights in enumerate(whole):
        which = (member - towards * away) % copies
        source = line // capacity * slots_host + which * capacity + line % capacity
        results.append(expert_rows(arrived, source, weights, hidden_width))

    line = jnp.arange(hosts * slots_host, dtype=jnp.int32)
    which = line % slots_host // capacity
    away = towards * (member - which) % copies
    source = away * taken + line // slots_host * capacity + line % capacity
    leaving = reorder_rows(results, source[:, None], hosts, slots_host)
    returned = [leaving[h] if h == 0 else lax.ppermute(leaving[h], "ep", back[h]) for h in range(hosts)]
    return mix_rows(returned, slots, route_weights, shared_result)


def solution(mesh):
    return jax.shard_map(
        on_device,
        mesh=mesh,
        in_specs=(
            P(("grp", "ep"), None),
            P(),
            P(("grp", "ep"), None),
            P(("grp", "ep"), None),
            P("ep", None, None),
            P("ep", None, None),
            P("ep", None, None),
            P(),
            P(),
            P(),
        ),
        out_specs=P(("grp", "ep"), None),
        check_vma=False,
    )
```

```python
import jax
import jax.numpy as jnp
from jax import lax
from jax.experimental import pallas as pl
from jax.experimental.pallas import tpu as pltpu
from jax.sharding import PartitionSpec as P


BLOCK = 4
CORES = 2
LIMIT = 48 * 1024 * 1024


def swiglu_rows(row_block, w_gate, w_up, w_down):
    gate_part = jnp.dot(row_block, w_gate, preferred_element_type=jnp.float32)
    up_part = jnp.dot(row_block, w_up, preferred_element_type=jnp.float32)
    hidden = (jax.nn.silu(gate_part) * up_part).astype(jnp.bfloat16)
    return jnp.dot(hidden, w_down, preferred_element_type=jnp.float32)


def call(body, out_shape, name, flops):
    return pl.pallas_call(
        body,
        out_shape=out_shape,
        name=name,
        compiler_params=pltpu.CompilerParams(vmem_limit_bytes=LIMIT),
        cost_estimate=pl.CostEstimate(flops=flops, bytes_accessed=8 << 20, transcendentals=0),
    )


def select_rows(normed, slots, count, rows):
    width = normed.shape[1]

    def body(slots_ref, normed_ref, *outs):
        slot_a, slot_b = slots_ref[0:1, :], slots_ref[1:2, :]
        for s in range(count):
            row = lax.broadcasted_iota(jnp.int32, (rows, normed.shape[0]), 0) + s * rows
            pick = jnp.where((row == slot_a) | (row == slot_b), 1.0, 0.0).astype(jnp.bfloat16)
            outs[s][...] = jnp.dot(pick, normed_ref[...], preferred_element_type=jnp.float32).astype(jnp.bfloat16)

    out = [jax.ShapeDtypeStruct((rows, width), jnp.bfloat16)] * count
    return call(body, out, "select_rows", 2 * count * rows * normed.shape[0] * width)(slots, normed)


def expert_rows(arrived, source, slabs, places, hidden_width):
    width = arrived[0].shape[1]
    total = len(arrived) * arrived[0].shape[0]
    rows = source.shape[0]
    cuts = [(n, i, size) for n, (slab, size) in enumerate(slabs) for i in range(slab.shape[0] // size)]
    count = len(slabs)

    def body(places_ref, source_ref, *refs):
        slab_refs, row_refs = refs[:count], refs[count:-3]
        out, weights_ref, sems = refs[-3:]
        copies = []
        for q, (n, i, size) in enumerate(cuts):
            to = pl.ds(pl.multiple_of(places_ref[q], size), size)
            copies.append(
                pltpu.make_async_copy(slab_refs[n].at[pl.ds(i * size, size)], weights_ref.at[to], sems.at[q])
            )
            copies[-1].start()
        everything = jnp.concatenate([ref[...] for ref in row_refs], axis=0)
        column = lax.broadcasted_iota(jnp.int32, (rows, total), 1)
        pick = jnp.where(column == source_ref[...], 1.0, 0.0).astype(jnp.bfloat16)
        mine = jnp.dot(pick, everything, preferred_element_type=jnp.float32).astype(jnp.bfloat16)
        for copy in copies:
            copy.wait()
        gate = jnp.dot(mine, weights_ref[0:width, :], preferred_element_type=jnp.float32)
        up = jnp.dot(mine, weights_ref[width : 2 * width, :], preferred_element_type=jnp.float32)
        hidden = (gate / (1.0 + jnp.exp(-gate)) * up).astype(jnp.bfloat16)
        for b in range(width // hidden_width):
            start = 2 * width + b * hidden_width
            down = weights_ref[start : start + hidden_width, :]
            part = jnp.dot(hidden, down, preferred_element_type=jnp.float32)
            out[:, b * hidden_width : (b + 1) * hidden_width] = part.astype(jnp.bfloat16)

    vmem = pl.BlockSpec(memory_space=pltpu.VMEM)
    return pl.pallas_call(
        body,
        out_shape=jax.ShapeDtypeStruct((rows, width), jnp.bfloat16),
        in_specs=[pl.BlockSpec(memory_space=pltpu.SMEM), vmem]
        + [pl.BlockSpec(memory_space=pl.ANY)] * count
        + [vmem] * len(arrived),
        out_specs=vmem,
        scratch_shapes=[pltpu.VMEM((3 * width, hidden_width), jnp.bfloat16), pltpu.SemaphoreType.DMA((len(cuts),))],
        name="expert_rows",
        compiler_params=pltpu.CompilerParams(vmem_limit_bytes=LIMIT),
        cost_estimate=pl.CostEstimate(
            flops=2 * rows * width * (total + 3 * hidden_width), bytes_accessed=6 << 20, transcendentals=0
        ),
    )(places, source, *[slab for slab, _ in slabs], *arrived)


def reorder_rows(results, source, count, rows):
    width = results[0].shape[1]
    total = len(results) * results[0].shape[0]

    def body(source_ref, *refs):
        everything = jnp.concatenate([ref[...] for ref in refs[: len(results)]], axis=0)
        for s in range(count):
            column = lax.broadcasted_iota(jnp.int32, (rows, total), 1)
            pick = jnp.where(column == source_ref[s * rows : (s + 1) * rows, :], 1.0, 0.0).astype(jnp.bfloat16)
            picked = jnp.dot(pick, everything, preferred_element_type=jnp.float32)
            refs[len(results) + s][...] = picked.astype(jnp.bfloat16)

    out = [jax.ShapeDtypeStruct((rows, width), jnp.bfloat16)] * count
    return call(body, out, "reorder_rows", 2 * count * rows * total * width)(source, *results)


def mix_rows(returned, slots, factors, shared_result):
    width = returned[0].shape[1]
    total = len(returned) * returned[0].shape[0]
    tok_rows, top_count = slots.shape

    def body(slots_ref, factors_ref, shared_ref, *refs):
        everything = jnp.concatenate([ref[...] for ref in refs[:-1]], axis=0)
        column = lax.broadcasted_iota(jnp.int32, (tok_rows, total), 1)
        spread = jnp.zeros((tok_rows, total), jnp.float32)
        for k in range(top_count):
            spread = spread + jnp.where(column == slots_ref[:, k : k + 1], factors_ref[:, k : k + 1], 0.0)
        high = spread.astype(jnp.bfloat16)
        low = (spread - high.astype(jnp.float32)).astype(jnp.bfloat16)
        routed = jnp.dot(high, everything, preferred_element_type=jnp.float32)
        routed = routed + jnp.dot(low, everything, preferred_element_type=jnp.float32)
        refs[-1][...] = (routed + shared_ref[...]).astype(jnp.bfloat16)

    out = jax.ShapeDtypeStruct((tok_rows, width), jnp.bfloat16)
    return call(body, out, "mix_rows", 4 * tok_rows * total * width)(slots, factors, shared_result, *returned)


def on_device(
    tokens,
    norm_gain,
    routes,
    route_weights,
    expert_gate,
    expert_up,
    expert_down,
    shared_gate,
    shared_up,
    shared_down,
):
    tok_rows, model_width = tokens.shape
    top_count = routes.shape[1]
    hidden_width = expert_gate.shape[2]
    devices_ep = lax.axis_size("ep")
    groups = lax.axis_size("grp")
    capacity = 5 * tok_rows * top_count // (4 * devices_ep)
    chips = devices_ep // CORES
    copies = chips // BLOCK
    hosts = BLOCK * CORES
    slots_host = copies * capacity
    me = lax.axis_index("ep")
    chip, core = me // CORES, me % CORES
    member = chip // BLOCK

    down_blocks = [expert_down[0, :, b * hidden_width : (b + 1) * hidden_width] for b in range(model_width // hidden_width)]
    stacked = jnp.concatenate([expert_gate[0], expert_up[0], *down_blocks], axis=0)
    share_rows = stacked.shape[0] // groups
    share = lax.dynamic_slice_in_dim(stacked, lax.axis_index("grp") * share_rows, share_rows, 0)

    onward = [(d, (d + (hosts if d % CORES == 0 else -hosts)) % devices_ep) for d in range(devices_ep)]
    upcast = tokens.astype(jnp.float32)
    factor = lax.rsqrt(jnp.mean(upcast * upcast, axis=-1, keepdims=True) + 1e-06)
    normed = (upcast * factor * norm_gain).astype(jnp.bfloat16)

    flat_expert = routes.reshape(-1)
    onehot = (flat_expert[:, None] == jnp.arange(devices_ep, dtype=jnp.int32)[None, :]).astype(jnp.int32)
    position = jnp.sum(jnp.cumsum(onehot, axis=0) * onehot, axis=1) - 1
    expert_chip = flat_expert // CORES
    turn = (expert_chip - chip) % BLOCK
    host = turn * CORES + (flat_expert + core) % CORES
    slot = host * slots_host + (expert_chip // BLOCK) * capacity + position
    slots = slot.reshape(tok_rows, top_count)

    def host_of(d, h):
        z, c = d // CORES, d % CORES
        turn, swap = h // CORES, h % CORES
        half = BLOCK // 2
        move = turn - BLOCK if turn > half or (turn == half and c == 1) else turn
        return (z + move) % chips * CORES + (c + swap) % CORES

    outgoing = select_rows(normed, slots.T, hosts, slots_host)
    arrived, back = [], []
    for h in range(hosts):
        there = [(d, host_of(d, h)) for d in range(devices_ep)]
        back.append([(b, a) for a, b in there])
        arrived.append(outgoing[h] if h == 0 else lax.ppermute(outgoing[h], "ep", there))

    inner = 1 << ((groups.bit_length() - 1) // 2)
    inner = inner if groups % inner == 0 else 1
    outer = groups // inner
    group = lax.axis_index("grp")

    def gather(value, along_inner):
        def shifted(step):
            if along_inner:
                return [(g, g // inner * inner + (g + step) % inner) for g in range(groups)]
            return [(g, (g + step * inner) % groups) for g in range(groups)]

        size = inner if along_inner else outer
        found, ahead, behind = [(0, value)], value, value
        for k in range(1, size // 2 + 1):
            ahead = lax.ppermute(ahead, "grp", shifted(1))
            found.append((k, ahead))
            if len(found) < size:
                behind = lax.ppermute(behind, "grp", shifted(-1))
                found.append((-k, behind))
        return found

    def joined(found):
        return [away for away, _ in found], jnp.concatenate([value for _, value in found], axis=0)

    def placed(aways, found, inner_first, size, start):
        spots = []
        for second, _ in found:
            for first in aways:
                i, o = (first, second) if inner_first else (second, first)
                spots.append(((group // inner - o) % outer * inner + (group % inner - i) % inner) * share_rows + start)
        return [(value, size) for _, value in found], spots

    taken = hosts * capacity
    towards = 1 - 2 * core
    line = jnp.arange(taken, dtype=jnp.int32)[:, None]
    half = share_rows // 2

    def expert(away, slabs, spots):
        which = (member - towards * away) % copies
        source = line // capacity * slots_host + which * capacity + line % capacity
        places = jnp.stack(spots).astype(jnp.int32)
        return expert_rows(arrived, source, slabs, places, hidden_width)

    results, first, second = [], {}, {}
    piece = share
    for step in range(copies + 2):
        made = []
        if step < copies - 1:
            moved = lax.ppermute(piece, "ep", onward)
            made.append(moved)
            first[step] = [(True, share_rows, 0, *joined(gather(piece, True)))]
        elif step == copies - 1:
            first[step] = [
                (True, half, 0, *joined(gather(piece[:half], True))),
                (False, half, half, *joined(gather(piece[half:], False))),
            ]
        if step - 1 in first:
            slabs, spots = [], []
            for inner_first, size, start, aways, value in first[step - 1]:
                more = placed(aways, gather(value, not inner_first), inner_first, size, start)
                slabs, spots = slabs + more[0], spots + more[1]
            second[step - 1] = (slabs, spots)
        if step - 2 in second:
            results.append(expert(step - 2, *second[step - 2]))
        flat = [made, [entry[-1] for entry in first.get(step, [])], [slab for slab, _ in second.get(step - 1, ((), ()))[0]]]
        flat.append(results[-1:] if step - 2 in second else [])
        if step == 1:
            flat.append(arrived)
        made, values, slabs, *rest = lax.optimization_barrier(flat)
        if made:
            piece = made[0]
        if step in first:
            first[step] = [(*entry[:-1], value) for entry, value in zip(first[step], values)]
        if step - 1 in second:
            old, spots = second[step - 1]
            second[step - 1] = ([(value, size) for value, (_, size) in zip(slabs, old)], spots)
        if rest[0]:
            results[-1] = rest[0][0]
        if step == 1:
            arrived = rest[1]

    shared_result = swiglu_rows(normed, shared_gate, shared_up, shared_down)

    line = jnp.arange(hosts * slots_host, dtype=jnp.int32)
    which = line % slots_host // capacity
    away = towards * (member - which) % copies
    source = away * taken + line // slots_host * capacity + line % capacity
    leaving = reorder_rows(results, source[:, None], hosts, slots_host)
    returned = [leaving[h] if h == 0 else lax.ppermute(leaving[h], "ep", back[h]) for h in range(hosts)]
    return mix_rows(returned, slots, route_weights, shared_result)


def solution(mesh):
    return jax.shard_map(
        on_device,
        mesh=mesh,
        in_specs=(
            P(("grp", "ep"), None),
            P(),
            P(("grp", "ep"), None),
            P(("grp", "ep"), None),
            P("ep", None, None),
            P("ep", None, None),
            P("ep", None, None),
            P(),
            P(),
            P(),
        ),
        out_specs=P(("grp", "ep"), None),
        check_vma=False,
    )
```

```python
import math

import jax
import jax.numpy as jnp
from jax import lax
from jax.experimental import pallas as pl
from jax.experimental.pallas import tpu as pltpu
from jax.sharding import PartitionSpec as P


BLOCK = 4
CORES = 2
TILE = 8
LIMIT = 48 * 1024 * 1024


def swiglu_rows(row_block, w_gate, w_up, w_down):
    gate_part = jnp.dot(row_block, w_gate, preferred_element_type=jnp.float32)
    up_part = jnp.dot(row_block, w_up, preferred_element_type=jnp.float32)
    hidden = (jax.nn.silu(gate_part) * up_part).astype(jnp.bfloat16)
    return jnp.dot(hidden, w_down, preferred_element_type=jnp.float32)


def call(body, out_shape, flops):
    return pl.pallas_call(
        body,
        out_shape=out_shape,
        compiler_params=pltpu.CompilerParams(vmem_limit_bytes=LIMIT),
        cost_estimate=pl.CostEstimate(flops=flops, bytes_accessed=8 << 20, transcendentals=0),
    )


def own_share(group, groups, gate, up, down):
    width, hidden_width = gate.shape
    rows = 3 * width // groups
    unit = math.gcd(rows, hidden_width)

    def body(group_ref, gate_ref, up_ref, down_ref, out, sems):
        for q in range(rows // unit):
            row = group_ref[0] * rows + q * unit
            to, sem = out.at[pl.ds(q * unit, unit)], sems.at[q]

            @pl.when(row < width)
            def _():
                at = pl.ds(pl.multiple_of(row, unit), unit)
                pltpu.make_async_copy(gate_ref.at[at], to, sem).start()

            @pl.when((row >= width) & (row < 2 * width))
            def _():
                at = pl.ds(pl.multiple_of(row - width, unit), unit)
                pltpu.make_async_copy(up_ref.at[at], to, sem).start()

            @pl.when(row >= 2 * width)
            def _():
                within = row - 2 * width
                at = pl.ds(pl.multiple_of(within % hidden_width, unit), unit)
                block = pl.ds(pl.multiple_of(within // hidden_width * hidden_width, hidden_width), hidden_width)
                pltpu.make_async_copy(down_ref.at[at, block], to, sem).start()

        for q in range(rows // unit):
            pltpu.make_async_copy(gate_ref.at[pl.ds(0, unit)], out.at[pl.ds(q * unit, unit)], sems.at[q]).wait()

    return pl.pallas_call(
        body,
        out_shape=jax.ShapeDtypeStruct((rows, hidden_width), jnp.bfloat16),
        in_specs=[pl.BlockSpec(memory_space=pltpu.SMEM)] + [pl.BlockSpec(memory_space=pl.ANY)] * 3,
        out_specs=pl.BlockSpec(memory_space=pltpu.VMEM),
        scratch_shapes=[pltpu.SemaphoreType.DMA((rows // unit,))],
        name="own_share",
        compiler_params=pltpu.CompilerParams(vmem_limit_bytes=LIMIT),
    )(group, gate, up, down)


def select_rows(normed, slots, count, rows):
    width = normed.shape[1]

    def body(slots_ref, normed_ref, *outs):
        slot_a, slot_b = slots_ref[0:1, :], slots_ref[1:2, :]
        for s in range(count):
            row = lax.broadcasted_iota(jnp.int32, (rows, normed.shape[0]), 0) + s * rows
            pick = jnp.where((row == slot_a) | (row == slot_b), 1.0, 0.0).astype(jnp.bfloat16)
            outs[s][...] = jnp.dot(pick, normed_ref[...], preferred_element_type=jnp.float32).astype(jnp.bfloat16)

    out = [jax.ShapeDtypeStruct((rows, width), jnp.bfloat16)] * count
    return call(body, out, 2 * count * rows * normed.shape[0] * width)(slots, normed)


def expert_rows(arrived, source, slabs, places, hidden_width):
    width = arrived[0].shape[1]
    total = len(arrived) * arrived[0].shape[0]
    rows = source.shape[0]
    cuts = [(n, i, size) for n, (slab, size) in enumerate(slabs) for i in range(slab.shape[0] // size)]
    count = len(slabs)

    def body(places_ref, source_ref, *refs):
        slab_refs, row_refs = refs[:count], refs[count:-3]
        out, weights_ref, sems = refs[-3:]
        copies = []
        for q, (n, i, size) in enumerate(cuts):
            to = pl.ds(pl.multiple_of(places_ref[q], size), size)
            copies.append(
                pltpu.make_async_copy(slab_refs[n].at[pl.ds(i * size, size)], weights_ref.at[to], sems.at[q])
            )
            copies[-1].start()
        everything = jnp.concatenate([ref[...] for ref in row_refs], axis=0)
        column = lax.broadcasted_iota(jnp.int32, (rows, total), 1)
        pick = jnp.where(column == source_ref[...], 1.0, 0.0).astype(jnp.bfloat16)
        mine = jnp.dot(pick, everything, preferred_element_type=jnp.float32).astype(jnp.bfloat16)
        for copy in copies:
            copy.wait()
        gate = jnp.dot(mine, weights_ref[0:width, :], preferred_element_type=jnp.float32)
        up = jnp.dot(mine, weights_ref[width : 2 * width, :], preferred_element_type=jnp.float32)
        hidden = (gate / (1.0 + jnp.exp(-gate)) * up).astype(jnp.bfloat16)
        for b in range(width // hidden_width):
            start = 2 * width + b * hidden_width
            down = weights_ref[start : start + hidden_width, :]
            part = jnp.dot(hidden, down, preferred_element_type=jnp.float32)
            out[:, b * hidden_width : (b + 1) * hidden_width] = part.astype(jnp.bfloat16)

    vmem = pl.BlockSpec(memory_space=pltpu.VMEM)
    return pl.pallas_call(
        body,
        out_shape=jax.ShapeDtypeStruct((rows, width), jnp.bfloat16),
        in_specs=[pl.BlockSpec(memory_space=pltpu.SMEM), vmem]
        + [pl.BlockSpec(memory_space=pl.ANY)] * count
        + [vmem] * len(arrived),
        out_specs=vmem,
        scratch_shapes=[pltpu.VMEM((3 * width, hidden_width), jnp.bfloat16), pltpu.SemaphoreType.DMA((len(cuts),))],
        name="expert_rows",
        compiler_params=pltpu.CompilerParams(vmem_limit_bytes=LIMIT),
        cost_estimate=pl.CostEstimate(
            flops=2 * rows * width * (total + 3 * hidden_width), bytes_accessed=6 << 20, transcendentals=0
        ),
    )(places, source, *[slab for slab, _ in slabs], *arrived)


def reorder_rows(results, count, capacity):
    size, width = results[0].shape
    total = len(results) * size
    rows = -(-len(results) * capacity // TILE) * TILE

    def body(*refs):
        everything = jnp.concatenate([ref[...] for ref in refs[: len(results)]], axis=0)
        line = lax.broadcasted_iota(jnp.int32, (rows, total), 0)
        column = lax.broadcasted_iota(jnp.int32, (rows, total), 1)
        base = line // capacity * size + line % capacity
        for s in range(count):
            hit = (column == base + s * capacity) & (line < len(results) * capacity)
            picked = jnp.dot(jnp.where(hit, 1.0, 0.0).astype(jnp.bfloat16), everything, preferred_element_type=jnp.float32)
            refs[len(results) + s][...] = picked.astype(jnp.bfloat16)

    out = [jax.ShapeDtypeStruct((rows, width), jnp.bfloat16)] * count
    return call(body, out, 2 * count * rows * total * width)(*results)


def mix_rows(returned, slots, factors, shared_result):
    width = returned[0].shape[1]
    total = sum(value.shape[0] for value in returned)
    tok_rows, top_count = slots.shape

    def body(slots_ref, factors_ref, shared_ref, *refs):
        everything = jnp.concatenate([ref[...] for ref in refs[:-1]], axis=0)
        column = lax.broadcasted_iota(jnp.int32, (tok_rows, total), 1)
        spread = jnp.zeros((tok_rows, total), jnp.float32)
        for k in range(top_count):
            spread = spread + jnp.where(column == slots_ref[:, k : k + 1], factors_ref[:, k : k + 1], 0.0)
        high = spread.astype(jnp.bfloat16)
        low = (spread - high.astype(jnp.float32)).astype(jnp.bfloat16)
        routed = jnp.dot(high, everything, preferred_element_type=jnp.float32)
        routed = routed + jnp.dot(low, everything, preferred_element_type=jnp.float32)
        refs[-1][...] = (routed + shared_ref[...]).astype(jnp.bfloat16)

    out = jax.ShapeDtypeStruct((tok_rows, width), jnp.bfloat16)
    return call(body, out, 4 * tok_rows * total * width)(slots, factors, shared_result, *returned)


def on_device(
    tokens,
    norm_gain,
    routes,
    route_weights,
    expert_gate,
    expert_up,
    expert_down,
    shared_gate,
    shared_up,
    shared_down,
):
    tok_rows, _ = tokens.shape
    top_count = routes.shape[1]
    hidden_width = expert_gate.shape[2]
    devices_ep = lax.axis_size("ep")
    groups = lax.axis_size("grp")
    capacity = 5 * tok_rows * top_count // (4 * devices_ep)
    chips = devices_ep // CORES
    copies = chips // BLOCK
    hosts = BLOCK * CORES
    slots_host = copies * capacity
    me = lax.axis_index("ep")
    chip, core = me // CORES, me % CORES
    member = chip // BLOCK

    group = lax.axis_index("grp")
    share = own_share(group.reshape(1).astype(jnp.int32), groups, expert_gate[0], expert_up[0], expert_down[0])
    share_rows = share.shape[0]

    onward = [(d, (d + (hosts if d % CORES == 0 else -hosts)) % devices_ep) for d in range(devices_ep)]
    upcast = tokens.astype(jnp.float32)
    factor = lax.rsqrt(jnp.mean(upcast * upcast, axis=-1, keepdims=True) + 1e-06)
    normed = (upcast * factor * norm_gain).astype(jnp.bfloat16)

    flat_expert = routes.reshape(-1)
    onehot = (flat_expert[:, None] == jnp.arange(devices_ep, dtype=jnp.int32)[None, :]).astype(jnp.int32)
    position = jnp.sum(jnp.cumsum(onehot, axis=0) * onehot, axis=1) - 1
    expert_chip = flat_expert // CORES
    turn = (expert_chip - chip) % BLOCK
    host = turn * CORES + (flat_expert + core) % CORES
    slot = host * slots_host + (expert_chip // BLOCK) * capacity + position
    slots = slot.reshape(tok_rows, top_count)
    early = copies - 2
    early_rows, late_rows = -(-early * capacity // TILE) * TILE, -(-2 * capacity // TILE) * TILE
    below = (turn > BLOCK // 2) | ((turn == BLOCK // 2) & (core == 1))
    host_member = (chip + jnp.where(below, turn - BLOCK, turn)) % chips // BLOCK
    nth = (1 - 2 * (flat_expert % CORES)) * (host_member - expert_chip // BLOCK) % copies
    home_early = host * early_rows + nth * capacity + position
    home_late = hosts * early_rows + host * late_rows + (nth - early) * capacity + position
    homes = jnp.where(nth < early, home_early, home_late).reshape(tok_rows, top_count)

    def host_of(d, h):
        z, c = d // CORES, d % CORES
        turn, swap = h // CORES, h % CORES
        half = BLOCK // 2
        move = turn - BLOCK if turn > half or (turn == half and c == 1) else turn
        return (z + move) % chips * CORES + (c + swap) % CORES

    outgoing = select_rows(normed, slots.T, hosts, slots_host)
    routes_there = [[(d, host_of(d, h)) for d in range(devices_ep)] for h in range(hosts)]
    routes_back = [[(b, a) for a, b in pairs] for pairs in routes_there]

    def sent(values, pairs):
        return [value if h == 0 else lax.ppermute(value, "ep", pairs[h]) for h, value in enumerate(values)]

    inner = 1 << ((groups.bit_length() - 1) // 2)
    inner = inner if groups % inner == 0 else 1
    outer = groups // inner

    def gather(value, along_inner):
        def shifted(step):
            if along_inner:
                return [(g, g // inner * inner + (g + step) % inner) for g in range(groups)]
            return [(g, (g + step * inner) % groups) for g in range(groups)]

        size = inner if along_inner else outer
        found, ahead, behind = [(0, value)], value, value
        for k in range(1, size // 2 + 1):
            ahead = lax.ppermute(ahead, "grp", shifted(1))
            found.append((k, ahead))
            if len(found) < size:
                behind = lax.ppermute(behind, "grp", shifted(-1))
                found.append((-k, behind))
        return found

    def joined(found):
        return [away for away, _ in found], jnp.concatenate([value for _, value in found], axis=0)

    def placed(aways, found, inner_first, size, start):
        spots = []
        for second, _ in found:
            for first in aways:
                i, o = (first, second) if inner_first else (second, first)
                spots.append(((group // inner - o) % outer * inner + (group % inner - i) % inner) * share_rows + start)
        return [(value, size) for _, value in found], spots

    taken = hosts * capacity
    towards = 1 - 2 * core
    line = jnp.arange(taken, dtype=jnp.int32)[:, None]
    half = share_rows // 2

    def expert(away, slabs, spots):
        which = (member - towards * away) % copies
        source = line // capacity * slots_host + which * capacity + line % capacity
        places = jnp.stack(spots).astype(jnp.int32)
        return expert_rows(arrived, source, slabs, places, hidden_width)

    total = 2 * copies
    pieces = {0: share[:half], 1: share[half:]}
    first, second, results, arrived = {}, {}, [], None
    before = {}
    for step in range(total + 3):
        made = {}
        if step < total - 2:
            made["piece"] = lax.ppermute(pieces[step], "ep", onward)
        if step in pieces:
            aways, value = joined(gather(pieces[step], step % 2 == 0))
            made["first"] = value
            first[step] = aways
        if step - 2 in first:
            made["second"] = gather(before["second_of"], step % 2 != 0)
        if step == 2:
            made["arrived"] = sent(outgoing, routes_there)
        k = step - 5
        if k >= 0 and k % 2 == 0 and k // 2 < copies - 1:
            both = [second[k], second[k + 1]]
            made["result"] = expert(k // 2, both[0][0] + both[1][0], both[0][1] + both[1][1])
        if step == total + 1:
            made["home"] = sent(reorder_rows(results[:early], hosts, capacity), routes_back)
        waited = dict(before.get("made", {}))
        if step == 1:
            waited["outgoing"] = outgoing
        finds = [away for away, _ in waited["second"]] if "second" in waited else None
        if finds is not None:
            waited["second"] = [value for _, value in waited["second"]]
        waited = lax.optimization_barrier(waited)
        if step == 1:
            outgoing = waited["outgoing"]
        if "piece" in waited:
            pieces[step + 1] = waited["piece"]
        if finds is not None:
            t = step - 3
            inner_first = t % 2 == 0
            found = list(zip(finds, waited["second"]))
            second[t] = placed(first[t], found, inner_first, half, t % 2 * half)
        if "arrived" in waited:
            arrived = waited["arrived"]
        if "result" in waited:
            results.append(waited["result"])
        if "home" in waited:
            home_early_rows = waited["home"]
        before = {"made": made, "second_of": waited.get("first")}

    k = total - 2
    results.append(expert(copies - 1, second[k][0] + second[k + 1][0], second[k][1] + second[k + 1][1]))
    returned = home_early_rows + sent(reorder_rows(results[early:], hosts, capacity), routes_back)
    shared_result = swiglu_rows(normed, shared_gate, shared_up, shared_down)
    return mix_rows(returned, homes, route_weights, shared_result)


def solution(mesh):
    return whole_program(mesh)


def whole_program(mesh):
    return jax.shard_map(
        on_device,
        mesh=mesh,
        in_specs=(
            P(("grp", "ep"), None),
            P(),
            P(("grp", "ep"), None),
            P(("grp", "ep"), None),
            P("ep", None, None),
            P("ep", None, None),
            P("ep", None, None),
            P(),
            P(),
            P(),
        ),
        out_specs=P(("grp", "ep"), None),
        check_vma=False,
    )
```
